32 devices in a mesh: sp: 8 (over z, x), tp: 4 (over y, core).
Axes of the slice: x: 2, y: 2, z: 4, core: 2. Of those that a mesh axis runs over, the one named last changes fastest.
Arguments:
- residual: bfloat16 [2048, 2048], P(('sp', 'tp')), may hold values from -6 to 6
- query_wide: bfloat16 [2048, 512], P('sp', 'tp'), may hold values from -8 to 8
- key_wide: bfloat16 [2048, 512], P('sp', 'tp'), may hold values from -8 to 8
- value_wide: bfloat16 [2048, 512], P('sp', 'tp'), may hold values from -6 to 6
- query_narrow: bfloat16 [2048, 512], P('sp', 'tp'), may hold values from -8 to 8
- key_narrow: bfloat16 [2048, 512], P('sp', 'tp'), may hold values from -8 to 8
- value_narrow: bfloat16 [2048, 512], P('sp', 'tp'), may hold values from -6 to 6
- gate_wide: float32 [2048, 4], P('sp', 'tp'), may hold values from -2 to 20
- gate_narrow: float32 [2048, 8], P('sp', 'tp'), may hold values from -2 to 20
- out_wide: bfloat16 [512, 2048], replicated, may hold values from -0.1875 to 0.1875
- out_narrow: bfloat16 [512, 2048], replicated, may hold values from -0.1875 to 0.1875
- norm_gain: float32 [2048], replicated, may hold values from 0.1 to 1.9
- routing: int32 [2048, 2], P(('sp', 'tp')), may hold values from 0 to 7, as said below
- route_weight: float32 [2048, 2], P(('sp', 'tp')), may hold values from 0.3 to 1.5
- gate_weight: bfloat16 [8, 2048, 1024], P('sp', None, 'tp'), may hold values from -0.125 to 0.125
- up_weight: bfloat16 [8, 2048, 1024], P('sp', None, 'tp'), may hold values from -0.125 to 0.125
- down_weight: bfloat16 [8, 1024, 2048], P('sp', 'tp'), may hold values from -0.1875 to 0.1875
Outputs:
- result: bfloat16 [2048, 2048], P(('sp', 'tp'))
The draws below stay inside these ranges and needn't reach their ends.
Inputs may be any that keep to these rules, and one draw needn't show every extreme that they name: `routing`: each row names 2 different experts of one group (experts g * 2 to g * 2 + 1). In each aligned block of 64 rows (the rows of one device) no expert is named by more than 32 rows; one group, the same for all blocks, has each of its experts named by exactly 32 rows of every block.
All inputs are finite; a program needn't handle non-finite values.
Results may differ from the reference program's by a relative error of at most 0.017.
Values may be sent and summed in bfloat16 or wider, within the bound.
A program may use at most 128 MiB of HBM per device.

```python
import math
import jax
import jax.numpy as jnp
from jax import lax

D = 2048
WIDE = 4
HW = 128
NARROW = 8
HN = 64
FFE = 1024
GROUPS = 4
TOP = 2
TOK_DEV = 256
TOKENS = 2048
EXPERTS = 8
EPG = 2
ROWS_DEV = 64
CAP = 32
N_TP = 4


def projected(key, breadth, salt_value):
    values = 1.7 * jax.random.normal(jax.random.fold_in(key, salt_value), (TOKENS, breadth), jnp.float32)
    values = jnp.clip(values, -8.0, 8.0)
    return values.astype(jnp.bfloat16)


def forget(key, head_count, salt_value):
    seeded = jax.random.fold_in(key, salt_value)
    order_key, drift_key, jitter_key = jax.random.split(seeded, 3)
    ranking = jax.random.permutation(order_key, head_count)
    keeping = head_count // 2
    baseline = jnp.where(ranking < keeping, jnp.log(1.0 * TOKENS), jnp.log(40.0))
    shards = TOKENS // TOK_DEV
    drift_part = jax.random.uniform(drift_key, (shards, 1, head_count), jnp.float32, -0.8, 0.8)
    drift_part = jnp.broadcast_to(drift_part, (shards, TOK_DEV, head_count)).reshape(TOKENS, head_count)
    jitter = jnp.clip(jax.random.normal(jitter_key, (TOKENS, head_count), jnp.float32), -4.0, 4.0)
    return (baseline[None, :] + drift_part + jitter).astype(jnp.float32)


def draw_query_wide(key, part):
    return projected(key, WIDE * HW, 11)


def draw_key_wide(key, part):
    return projected(key, WIDE * HW, 12)


def draw_query_narrow(key, part):
    return projected(key, NARROW * HN, 21)


def draw_key_narrow(key, part):
    return projected(key, NARROW * HN, 22)


def draw_gate_wide(key, part):
    return forget(key, WIDE, 31)


def draw_gate_narrow(key, part):
    return forget(key, NARROW, 32)


def route_block(key, full_group):
    cut_key, label_key, row_key = jax.random.split(key, 3)
    half_rows = ROWS_DEV // 2
    ordinal = jnp.arange(ROWS_DEV, dtype=jnp.int32)
    cut_points = jnp.sort(jax.random.randint(cut_key, (GROUPS - 2,), 0, half_rows + 1))
    remainder = ordinal - half_rows
    other_group = jnp.sum((remainder[:, None] >= cut_points[None, :]).astype(jnp.int32), axis=1)
    group_starts = jnp.concatenate([jnp.zeros((1,), jnp.int32), cut_points.astype(jnp.int32)])
    in_full = ordinal < half_rows
    ranking = jnp.where(in_full, ordinal, remainder - group_starts[other_group])
    chosen_group = jnp.where(in_full, full_group, (full_group + 1 + other_group) % GROUPS)

    def labels_of(group_number):
        return jax.random.permutation(jax.random.fold_in(label_key, group_number), EPG)
    labels = jax.vmap(labels_of)(jnp.arange(GROUPS, dtype=jnp.int32))
    slot_number = TOP * ranking[:, None] + jnp.arange(TOP, dtype=jnp.int32)[None, :]
    local_expert = labels[chosen_group[:, None], slot_number % EPG]
    expert_ids = (chosen_group[:, None] * EPG + local_expert).astype(jnp.int32)
    shuffled = jax.random.permutation(row_key, ROWS_DEV)
    return jnp.zeros((ROWS_DEV, TOP), jnp.int32).at[shuffled].set(expert_ids)


def draw_routing(key, part):
    seeded = jax.random.fold_in(key, 4242)
    full_group = jax.random.randint(jax.random.fold_in(seeded, 1), (), 0, GROUPS)

    def one_block(block_number):
        return route_block(jax.random.fold_in(seeded, block_number + 2), full_group)
    blocks = jax.vmap(one_block)(jnp.arange(TOKENS // ROWS_DEV, dtype=jnp.int32))
    return blocks.reshape(TOKENS, TOP)


def block_scale(own_key, dims, cuts, low, largest):
    loudness, own = 1.0, jax.random.fold_in(own_key, 6)
    for axis_at, shards_of in cuts:
        heights = jnp.exp(jax.random.uniform(jax.random.fold_in(own, axis_at), (shards_of,), jnp.float32, low / len(cuts), largest / len(cuts)))
        loudness = loudness * jnp.repeat(heights, dims[axis_at] // shards_of).reshape([-1 if axis == axis_at else 1 for axis in range(len(dims))])
    return loudness


def bell_draw(stream_key, shape, scale, most, cuts=(), kind=jnp.bfloat16):
    array = jax.random.normal(stream_key, shape, jnp.float32) * scale
    if len(cuts) > 0:
        array = block_scale(stream_key, shape, cuts, -0.22, 0.18) * array
    return jnp.clip(array, min=-most, max=most).astype(kind)


def setup_inputs(seed: int = 0) -> dict:
    key_list = jax.random.split(jax.random.key(seed), 18)
    return {
        "residual": bell_draw(key_list[0], (TOKENS, D), 1.0, 6.0, ((0, 32),)),
        "query_wide": draw_query_wide(jax.random.fold_in(key_list[17], 71), 0),
        "key_wide": draw_key_wide(jax.random.fold_in(key_list[17], 71), 0),
        "value_wide": bell_draw(key_list[3], (TOKENS, WIDE * HW), 1.0, 6.0, ((0, 8), (1, 4))),
        "query_narrow": draw_query_narrow(jax.random.fold_in(key_list[17], 71), 0),
        "key_narrow": draw_key_narrow(jax.random.fold_in(key_list[17], 71), 0),
        "value_narrow": bell_draw(key_list[6], (TOKENS, NARROW * HN), 1.0, 6.0, ((0, 8), (1, 4))),
        "gate_wide": draw_gate_wide(jax.random.fold_in(key_list[17], 71), 0),
        "gate_narrow": draw_gate_narrow(jax.random.fold_in(key_list[17], 71), 0),
        "out_wide": bell_draw(key_list[9], (WIDE * HW, D), (WIDE * HW + NARROW * HN) ** -0.5, 0.1875),
        "out_narrow": bell_draw(key_list[10], (NARROW * HN, D), (WIDE * HW + NARROW * HN) ** -0.5, 0.1875),
        "norm_gain": jnp.clip(1.0 + 0.18 * jax.random.normal(key_list[11], (D,), jnp.float32), 0.1, 1.9),
        "routing": draw_routing(jax.random.fold_in(key_list[17], 71), 0),
        "route_weight": jnp.clip(jnp.exp(math.log(1.5) - 1.60943787 * jax.random.uniform(key_list[13], (TOKENS, TOP), jnp.float32) ** block_scale(key_list[13], (TOKENS, TOP), ((0, 32),), -0.2, 0.2)), 0.3, 1.5),
        "gate_weight": bell_draw(key_list[14], (EXPERTS, D, FFE), D ** -0.5, 0.125, ((0, 8), (2, 4))),
        "up_weight": bell_draw(key_list[15], (EXPERTS, D, FFE), D ** -0.5, 0.125, ((0, 8), (2, 4))),
        "down_weight": bell_draw(key_list[16], (EXPERTS, FFE, D), FFE ** -0.5, 0.1875, ((0, 8), (1, 4))),
    }


epsilon = 1e-06

def attend(queries, keys, values, gates, head_width):
    length = queries.shape[0]
    head_count = gates.shape[1]
    decay = jnp.cumsum(jax.nn.log_sigmoid(gates.astype(jnp.float32)), axis=0)
    grid_query = queries.reshape(length, head_count, head_width).astype(jnp.float32)
    grid_key = keys.reshape(length, head_count, head_width).astype(jnp.float32)
    grid_value = values.reshape(length, head_count, head_width).astype(jnp.float32)
    block_size = math.gcd(length, 512)
    key_place = jnp.arange(length, dtype=jnp.int32)

    def one_block(position):
        begin = (position * block_size).astype(jnp.int32)
        part_query = lax.dynamic_slice_in_dim(grid_query, begin, block_size, 0)
        part_decay = lax.dynamic_slice_in_dim(decay, begin, block_size, 0)
        scores = jnp.einsum('thd,phd->htp', part_query, grid_key) * head_width ** (-0.5)
        scores = scores + part_decay.T[:, :, None] - decay.T[:, None, :]
        query_place = begin + jnp.arange(block_size, dtype=jnp.int32)
        scores = jnp.where(key_place[None, None, :] <= query_place[None, :, None], scores, -jnp.inf)
        weights = jnp.exp(scores - lax.optimization_barrier(jnp.max(scores, axis=2, keepdims=True)))
        weight_sum = lax.optimization_barrier(jnp.sum(weights, axis=2))
        rounded = lax.optimization_barrier(weights.astype(jnp.bfloat16)).astype(jnp.float32)
        mixed_heads = jnp.einsum('htp,phd->htd', rounded, grid_value) / weight_sum[:, :, None]
        return jnp.transpose(mixed_heads, (1, 0, 2)).reshape(block_size, head_count * head_width).astype(jnp.bfloat16)
    blocks = lax.map(one_block, jnp.arange(length // block_size, dtype=jnp.int32))
    return blocks.reshape(length, head_count * head_width)

def experts_apply(normed, routing, route_weight, gate_weight, up_weight, down_weight):
    length = normed.shape[0]
    chosen_count = routing.shape[1]
    expert_count = gate_weight.shape[0]
    flat_routes = routing.reshape(-1).astype(jnp.int32)
    matches = (flat_routes[:, None] == jnp.arange(expert_count, dtype=jnp.int32)[None, :]).astype(jnp.int32)
    ranking = lax.optimization_barrier(jnp.sum((jnp.cumsum(matches, axis=0) - matches) * matches, axis=1)).astype(jnp.int32)
    capacity_all = length // ROWS_DEV * CAP
    lookup = jnp.full((expert_count, capacity_all), length * chosen_count, jnp.int32)
    lookup = lookup.at[flat_routes, ranking].set(jnp.arange(length * chosen_count, dtype=jnp.int32))
    flat_weights = route_weight.reshape(-1)

    def one_expert(carried, pieces):
        copies, gate_part, up_part, down_part = pieces
        positions = (copies // chosen_count).astype(jnp.int32)
        chosen_rows = jnp.take(normed, positions, axis=0, mode='clip')
        gate_value = jnp.dot(chosen_rows, gate_part, preferred_element_type=jnp.float32)
        up_value = jnp.dot(chosen_rows, up_part, preferred_element_type=jnp.float32)
        hidden = (jax.nn.silu(gate_value) * up_value).astype(jnp.bfloat16)
        hidden_blocks = hidden.reshape(capacity_all, N_TP, -1).astype(jnp.float32)
        down_blocks = down_part.reshape(N_TP, -1, down_part.shape[1]).astype(jnp.float32)
        partial_out = jnp.einsum('lnf,nfd->nld', hidden_blocks, down_blocks)
        partial_out = lax.optimization_barrier(partial_out.astype(jnp.bfloat16)).astype(jnp.float32)
        expert_out = lax.optimization_barrier(jnp.sum(partial_out, axis=0)).astype(jnp.bfloat16)
        scale = jnp.take(flat_weights, copies, mode='fill', fill_value=0.0)
        carried = carried.at[positions].add(scale[:, None] * expert_out.astype(jnp.float32), mode='drop')
        return (carried, None)
    start = jnp.zeros((length, normed.shape[1]), jnp.float32)
    total, _ = lax.scan(one_expert, start, (lookup, gate_weight, up_weight, down_weight))
    return total

def reference(residual, query_wide, key_wide, value_wide, query_narrow, key_narrow, value_narrow, gate_wide, gate_narrow, out_wide, out_narrow, norm_gain, routing, route_weight, gate_weight, up_weight, down_weight):
    att_wide = attend(query_wide, key_wide, value_wide, gate_wide, HW)
    att_narrow = attend(query_narrow, key_narrow, value_narrow, gate_narrow, HN)
    mixed = jnp.dot(att_wide, out_wide, preferred_element_type=jnp.float32)
    mixed = mixed + jnp.dot(att_narrow, out_narrow, preferred_element_type=jnp.float32)
    middle = (residual.astype(jnp.float32) + mixed).astype(jnp.bfloat16)
    middle_wide = middle.astype(jnp.float32)
    spread = lax.optimization_barrier(jnp.mean(middle_wide * middle_wide, axis=1, keepdims=True))
    normed = (middle_wide * lax.rsqrt(spread + epsilon) * norm_gain).astype(jnp.bfloat16)
    routed = experts_apply(normed, routing, route_weight, gate_weight, up_weight, down_weight)
    return (middle_wide + routed).astype(jnp.bfloat16)
```

```python
import functools
import math

import jax
import jax.numpy as jnp
from jax import lax
from jax.experimental import pallas as pl
from jax.experimental.pallas import tpu as pltpu
from jax.sharding import PartitionSpec as P

HW = 128
HN = 64
GROUPS = 4


epsilon = 1e-06


def globalize(pieces, shard_rows):
    shards = pieces.shape[0] // shard_rows
    grid = pieces.reshape(shards, shard_rows, pieces.shape[1])
    endings = grid[:, -1, :]
    offsets = jnp.cumsum(endings, axis=0) - endings
    return (grid + offsets[:, None, :]).reshape(pieces.shape)


def head_block(
    state, queries, query_decay, keys, values, key_decay, first_key, first_query, head_width
):
    highest_old, weight_sum, weighted = state
    query_rows = queries.shape[0]
    head_count = query_decay.shape[1]
    key_rows = keys.shape[0]
    grid_query = queries.reshape(query_rows, head_count, head_width)
    grid_key = keys.reshape(key_rows, head_count, head_width)
    grid_value = values.reshape(key_rows, head_count, head_width)
    scores = jnp.einsum("thd,phd->htp", grid_query, grid_key, preferred_element_type=jnp.float32)
    scores = scores * head_width ** (-0.5) + query_decay.T[:, :, None] - key_decay.T[:, None, :]
    query_place = first_query + jnp.arange(query_rows, dtype=jnp.int32)
    key_place = first_key + jnp.arange(key_rows, dtype=jnp.int32)
    scores = jnp.where(key_place[None, None, :] <= query_place[None, :, None], scores, -jnp.inf)
    highest = jnp.maximum(highest_old, jnp.max(scores, axis=2))
    weights = jnp.exp(scores - highest[:, :, None])
    shrink = jnp.exp(highest_old - highest)
    weight_sum = weight_sum * shrink + jnp.sum(weights, axis=2)
    product = jnp.einsum(
        "htp,phd->htd", weights.astype(jnp.bfloat16), grid_value, preferred_element_type=jnp.float32
    )
    weighted = weighted * shrink[:, :, None] + product
    return (highest, weight_sum, weighted)


def fresh_state(head_count, shard_rows, head_width):
    return (
        jnp.full((head_count, shard_rows), -1e30, jnp.float32),
        jnp.zeros((head_count, shard_rows), jnp.float32),
        jnp.zeros((head_count, shard_rows, head_width), jnp.float32),
    )


def finish(state, shard_rows):
    highest, weight_sum, weighted = state
    mixed_heads = weighted / weight_sum[:, :, None]
    joined = jnp.transpose(mixed_heads, (1, 0, 2))
    return joined.reshape(shard_rows, weighted.shape[0] * weighted.shape[2]).astype(jnp.bfloat16)


def body(
    residual,
    query_wide,
    key_wide,
    value_wide,
    query_narrow,
    key_narrow,
    value_narrow,
    gate_wide,
    gate_narrow,
    out_wide,
    out_narrow,
    norm_gain,
    routing,
    route_weight,
    gate_weight,
    up_weight,
    down_weight,
):
    shard_rows = query_wide.shape[0]
    half_rows = shard_rows // 2
    sp_place = lax.axis_index("sp")
    first_query = sp_place * shard_rows
    running_wide = jnp.cumsum(jax.nn.log_sigmoid(gate_wide), axis=0)
    running_narrow = jnp.cumsum(jax.nn.log_sigmoid(gate_narrow), axis=0)
    pieces_wide, pieces_narrow = (
        lax.all_gather(running_wide, "sp", axis=0, tiled=True),
        lax.all_gather(running_narrow, "sp", axis=0, tiled=True),
    )
    every_wide = globalize(pieces_wide, shard_rows)
    every_narrow = globalize(pieces_narrow, shard_rows)
    late_first = first_query + half_rows
    halves = []
    for place, part_wide, part_narrow in (
        (first_query, query_wide[:half_rows], query_narrow[:half_rows]),
        (late_first, query_wide[half_rows:], query_narrow[half_rows:]),
    ):
        halves.append(
            (
                place,
                part_wide,
                part_narrow,
                lax.dynamic_slice_in_dim(every_wide, place, half_rows, 0),
                lax.dynamic_slice_in_dim(every_narrow, place, half_rows, 0),
            )
        )

    def half_state():
        return (
            fresh_state(gate_wide.shape[1], half_rows, HW),
            fresh_state(gate_narrow.shape[1], half_rows, HN),
        )

    state = (half_state(), half_state())
    keys_wide = lax.all_gather(key_wide, "sp", axis=0, tiled=True)
    values_wide = lax.all_gather(value_wide, "sp", axis=0, tiled=True)
    keys_narrow = lax.all_gather(key_narrow, "sp", axis=0, tiled=True)
    values_narrow = lax.all_gather(value_narrow, "sp", axis=0, tiled=True)
    span_rows = keys_wide.shape[0]
    block_size = math.gcd(span_rows, 2048)

    def visit(carried, position):
        inside = position * block_size

        def take_block(source):
            return lax.dynamic_slice_in_dim(source, inside, block_size, 0)

        def take_decay(source):
            return lax.dynamic_slice_in_dim(source, inside, block_size, 0)

        block_kw = take_block(keys_wide)
        block_vw = take_block(values_wide)
        block_kn = take_block(keys_narrow)
        block_vn = take_block(values_narrow)
        block_dw = take_decay(every_wide)
        block_dn = take_decay(every_narrow)

        def one_half(current, half):
            place, part_wide, part_narrow, query_decay_wide, query_decay_narrow = half

            def work(inner):
                first = head_block(
                    inner[0],
                    part_wide,
                    query_decay_wide,
                    block_kw,
                    block_vw,
                    block_dw,
                    inside,
                    place,
                    HW,
                )
                second = head_block(
                    inner[1],
                    part_narrow,
                    query_decay_narrow,
                    block_kn,
                    block_vn,
                    block_dn,
                    inside,
                    place,
                    HN,
                )
                return (first, second)

            def skip(inner):
                return inner

            return lax.cond(inside <= place + half_rows - 1, work, skip, current)

        updated = (one_half(carried[0], halves[0]), one_half(carried[1], halves[1]))
        return (updated, None)

    state, _ = lax.scan(visit, state, jnp.arange(span_rows // block_size, dtype=jnp.int32))
    att_wide = jnp.concatenate(
        [finish(state[0][0], half_rows), finish(state[1][0], half_rows)], axis=0
    )
    att_narrow = jnp.concatenate(
        [finish(state[0][1], half_rows), finish(state[1][1], half_rows)], axis=0
    )
    own_rows = residual.shape[0]
    tp_place = lax.axis_index("tp")
    rows_wide = lax.dynamic_slice_in_dim(
        out_wide, tp_place * att_wide.shape[1], att_wide.shape[1], 0
    )
    rows_narrow = lax.dynamic_slice_in_dim(
        out_narrow, tp_place * att_narrow.shape[1], att_narrow.shape[1], 0
    )
    first = jnp.dot(att_wide, rows_wide, preferred_element_type=jnp.float32)
    second = jnp.dot(att_narrow, rows_narrow, preferred_element_type=jnp.float32)
    mixed = lax.psum_scatter(
        (first + second).astype(jnp.bfloat16), "tp", scatter_dimension=0, tiled=True
    ).astype(jnp.float32)
    middle = (residual.astype(jnp.float32) + mixed).astype(jnp.bfloat16)
    middle_wide = middle.astype(jnp.float32)
    spread = jnp.mean(middle_wide * middle_wide, axis=1, keepdims=True)
    normed = (middle_wide * lax.rsqrt(spread + epsilon) * norm_gain).astype(jnp.bfloat16)
    features = normed.shape[1]
    chosen_count = routing.shape[1]
    expert_count = gate_weight.shape[0] * lax.axis_size("sp")
    capacity = own_rows * GROUPS // expert_count
    flat_routes = routing.reshape(-1)
    matches = (flat_routes[:, None] == jnp.arange(expert_count, dtype=jnp.int32)[None, :]).astype(
        jnp.int32
    )
    ranking = jnp.sum((jnp.cumsum(matches, axis=0) - matches) * matches, axis=1)
    placing = flat_routes * capacity + ranking
    picker = (
        placing[None, :] == jnp.arange(expert_count * capacity, dtype=jnp.int32)[:, None]
    ).astype(jnp.bfloat16)
    picker = jnp.sum(picker.reshape(expert_count * capacity, own_rows, chosen_count), axis=2)
    outgoing = jnp.dot(picker, normed, preferred_element_type=jnp.float32).astype(jnp.bfloat16)
    outgoing = outgoing.reshape(expert_count, capacity, features)
    arrived = lax.all_to_all(outgoing, "sp", split_axis=0, concat_axis=0, tiled=True)
    pooled = lax.all_gather(arrived.reshape(-1, features), "tp", axis=0, tiled=True)
    gate_value = jnp.dot(pooled, gate_weight[0], preferred_element_type=jnp.float32)
    up_value = jnp.dot(pooled, up_weight[0], preferred_element_type=jnp.float32)
    hidden = (jax.nn.silu(gate_value) * up_value).astype(jnp.bfloat16)
    answers = lax.psum_scatter(
        jnp.dot(hidden, down_weight[0], preferred_element_type=jnp.float32).astype(jnp.bfloat16),
        "tp",
        scatter_dimension=0,
        tiled=True,
    )
    returned = lax.all_to_all(
        answers.reshape(expert_count, capacity, features),
        "sp",
        split_axis=0,
        concat_axis=0,
        tiled=True,
    )
    picked = jnp.take(returned.reshape(expert_count * capacity, features), placing, axis=0)
    picked = picked.reshape(own_rows, chosen_count, features).astype(jnp.float32)
    combined = jnp.sum(route_weight[:, :, None] * picked, axis=1)
    return (middle_wide + combined).astype(jnp.bfloat16)


CORES = 2
MESH = pl.DeviceIdType.MESH
VMEM = pl.BlockSpec(memory_space=pltpu.VMEM)


def greet(peers):
    barrier = pltpu.get_barrier_semaphore()
    for peer in peers:
        pl.semaphore_signal(barrier, inc=1, device_id=peer, device_id_type=MESH)
    pl.semaphore_wait(barrier, len(peers))


def remote(source, target, send, receive, peer):
    return pltpu.make_async_remote_copy(
        src_ref=source,
        dst_ref=target,
        send_sem=send,
        recv_sem=receive,
        device_id=peer,
        device_id_type=MESH,
    )


def call(kernel, number, outs, scratch, args):
    return pl.pallas_call(
        kernel,
        out_shape=outs,
        in_specs=[VMEM] * len(args),
        out_specs=[VMEM] * len(outs),
        scratch_shapes=scratch,
        compiler_params=pltpu.CompilerParams(collective_id=number, has_side_effects=True),
    )(*args)


DMA = pltpu.SemaphoreType.DMA


def keys_kernel(outer, inner, count, *refs):
    ins, outs = refs[:count], refs[count : 2 * count]
    local, send_up, take_up, send_in, take_in = refs[2 * count :]
    place = lax.axis_index("sp")
    o, i = place // inner, place % inner
    tp = lax.axis_index("tp")

    def at(o_, i_):
        return (o_ * inner + i_, tp)

    greet(
        [at((o + d) % outer, i) for d in range(1, outer)]
        + [at(o, (i + d) % inner) for d in range(1, inner)]
    )
    other = at((o + 1) % outer, i)

    def up(t, a):
        slot = (o - t) * inner + i
        source = ins[a] if t == 0 else outs[a].at[slot]
        return remote(source, outs[a].at[slot], send_up.at[t, a], take_up.at[t, a], at(o + 1, i))

    def across(t, d, a):
        slot = (o - t) * inner + i
        source = ins[a] if t == 0 else outs[a].at[slot]
        return remote(
            source,
            outs[a].at[slot],
            send_in.at[t, d - 1, a],
            take_in.at[t, d - 1, a],
            at(o, (i + d) % inner),
        )

    def landed(slot, a, semaphore):
        remote(outs[a].at[slot], outs[a].at[slot], semaphore, semaphore, other).wait_recv()

    for a in range(count):
        pltpu.make_async_copy(ins[a], outs[a].at[place], local.at[a]).start()
    for t in range(outer):

        @pl.when(o >= t)
        def _(t=t):
            for a in range(count):
                if t > 0:
                    landed((o - t) * inner + i, a, take_up.at[t - 1, a])
                if t < outer - 1:

                    @pl.when(o + 1 < outer)
                    def _(a=a):
                        up(t, a).start()

                for d in range(1, inner):
                    if t > 0:
                        across(t, d, a).start()
                    else:

                        @pl.when((i + d) % inner > i)
                        def _(a=a, d=d):
                            across(t, d, a).start()

    for t in range(outer):

        @pl.when(o >= t)
        def _(t=t):
            for a in range(count):
                for d in range(1, inner):
                    giver = (i - d + inner) % inner
                    slot = (o - t) * inner + giver
                    if t > 0:
                        landed(slot, a, take_in.at[t, d - 1, a])
                        across(t, d, a).wait_send()
                    else:

                        @pl.when(giver < i)
                        def _(a=a, d=d, slot=slot):
                            landed(slot, a, take_in.at[0, d - 1, a])

                        @pl.when((i + d) % inner > i)
                        def _(a=a, d=d):
                            across(0, d, a).wait_send()

                if t < outer - 1:

                    @pl.when(o + 1 < outer)
                    def _(a=a):
                        up(t, a).wait_send()

    for a in range(count):
        pltpu.make_async_copy(ins[a], outs[a].at[place], local.at[a]).wait()


def gather_keys(arrays, outer, inner):
    count = len(arrays)
    outs = [jax.ShapeDtypeStruct((outer * inner,) + x.shape, x.dtype) for x in arrays]
    scratch = [
        DMA((count,)),
        DMA((outer, count)),
        DMA((outer, count)),
        DMA((outer, inner, count)),
        DMA((outer, inner, count)),
    ]
    return call(functools.partial(keys_kernel, outer, inner, count), 1, outs, scratch, arrays)


def attend_kernel(qw, qn, near, kw, vw, kn, vn, far, out, top, total, mixed):
    place = lax.axis_index("sp")
    rows = qw.shape[0]
    width = qn.shape[1]
    heads = 1 + width // HN
    lanes = lax.broadcasted_iota(jnp.int32, (rows, width), 1) // HN

    def query(h):
        if h == 0:
            return qw[...]
        return jnp.where(lanes == h - 1, qn[...], jnp.zeros_like(qn[...]))

    def block(j, shift, diagonal):
        for h in range(heads):
            keys, values = (kw, vw) if h == 0 else (kn, vn)
            size = HW if h == 0 else HN
            scores = lax.dot_general(
                query(h), keys[j], (((1,), (1,)), ((), ())), preferred_element_type=jnp.float32
            )
            drop = (near[:, h : h + 1] + shift[h]) - far[j, h : h + 1, :]
            scores = scores * size ** (-0.5) + drop
            if diagonal:
                t = lax.broadcasted_iota(jnp.int32, scores.shape, 0)
                s = lax.broadcasted_iota(jnp.int32, scores.shape, 1)
                scores = jnp.where(s <= t, scores, -jnp.inf)
            peak = jnp.max(scores, axis=1, keepdims=True)
            if diagonal:
                weights = jnp.exp(scores - peak)
                total[h] = jnp.sum(weights, axis=1, keepdims=True)
                mixed[h] = jnp.dot(
                    weights.astype(jnp.bfloat16), values[j], preferred_element_type=jnp.float32
                )
                top[h] = peak
            else:
                before = top[h]
                peak = jnp.maximum(before, peak)
                weights = jnp.exp(scores - peak)
                shrink = jnp.exp(before - peak)
                total[h] = total[h] * shrink + jnp.sum(weights, axis=1, keepdims=True)
                mixed[h] = mixed[h] * shrink + jnp.dot(
                    weights.astype(jnp.bfloat16), values[j], preferred_element_type=jnp.float32
                )
                top[h] = peak

    block(place, [jnp.zeros((1, 1), jnp.float32)] * heads, True)

    def step(t, shift):
        j = place - 1 - t
        shift = tuple(shift[h] + far[j, h : h + 1, rows - 1 : rows] for h in range(heads))
        block(j, shift, False)
        return shift

    lax.fori_loop(0, place, step, tuple(jnp.zeros((1, 1), jnp.float32) for _ in range(heads)))
    out[:, : qw.shape[1]] = (mixed[0] / total[0]).astype(jnp.bfloat16)
    narrow = mixed[1] / total[1]
    for h in range(2, heads):
        narrow = jnp.where(lanes == h - 1, mixed[h] / total[h], narrow)
    out[:, qw.shape[1] :] = narrow.astype(jnp.bfloat16)


def swap_kernel(axis, n, stride, source, target, local, send, take):
    sp, tp = lax.axis_index("sp"), lax.axis_index("tp")
    me = (sp if axis == "sp" else tp) // stride
    rest = (sp if axis == "sp" else tp) % stride

    def at(k):
        return (k * stride + rest, tp) if axis == "sp" else (sp, k * stride + rest)

    greet([at((me + d) % n) for d in range(1, n)])

    def copy(d):
        k = (me + d) % n
        return remote(source.at[k], target.at[me], send.at[d], take.at[d], at(k))

    for d in range(1, n):
        copy(d).start()
    own = pltpu.make_async_copy(source.at[me], target.at[me], local.at[0])
    own.start()
    own.wait()
    for d in range(1, n):
        slot = target.at[(me - d + n) % n]
        remote(slot, slot, send.at[d], take.at[d], at((me + d) % n)).wait_recv()
        copy(d).wait_send()


def swap(array, axis, n, stride, number):
    return call(
        functools.partial(swap_kernel, axis, n, stride),
        number,
        [jax.ShapeDtypeStruct(array.shape, array.dtype)],
        [DMA((1,)), DMA((n,)), DMA((n,))],
        [array],
    )[0]


def spread_kernel(outer, inner, ys, count, *refs):
    ins, outs = refs[:count], refs[count : 2 * count]
    local, send_a, take_a, send_b, take_b, send_c, take_c = refs[2 * count :]
    place, tp = lax.axis_index("sp"), lax.axis_index("tp")
    o, i, y, c = place // inner, place % inner, tp // CORES, tp % CORES
    steps = [(di, dy) for di in range(inner) for dy in range(ys) if (di, dy) != (0, 0)]
    mate = (place, y * CORES + 1 - c)

    def beside(di, dy):
        return (o * inner + (i + di) % inner, (y + dy) % ys * CORES + c)

    def above(d):
        return ((o + d) % outer * inner + i, tp)

    greet(
        [above(d) for d in range(1, outer)] + [beside(di, dy) for di, dy in steps] + [mate]
    )

    def slot(a, core, t, di, dy):
        return outs[a].at[
            core, (o - t + outer) % outer, (i - di + inner) % inner, (y - dy + ys) % ys
        ]

    def first(d, a):
        return remote(
            ins[a].at[(o + d) % outer],
            outs[a].at[c, o, i, y],
            send_a.at[d, a],
            take_a.at[d, a],
            above(d),
        )

    def second(t, di, dy, a):
        source = ins[a].at[o] if t == 0 else slot(a, c, t, 0, 0)
        return remote(
            source,
            slot(a, c, t, 0, 0),
            send_b.at[t, di, dy, a],
            take_b.at[t, di, dy, a],
            beside(di, dy),
        )

    def third(t, di, dy, a):
        source = ins[a].at[o] if (t, di, dy) == (0, 0, 0) else slot(a, c, t, di, dy)
        return remote(
            source, slot(a, c, t, di, dy), send_c.at[t, di, dy, a], take_c.at[t, di, dy, a], mate
        )

    def landed(where, semaphore):
        remote(where, where, semaphore, semaphore, mate).wait_recv()

    def relay(t):
        for di, dy in steps:
            for a in range(count):
                landed(slot(a, c, t, di, dy), take_b.at[t, di, dy, a])
                third(t, di, dy, a).start()

    for d in range(1, outer):
        for a in range(count):
            first(d, a).start()
    for t in range(outer):
        for a in range(count):
            if t == 0:
                pltpu.make_async_copy(ins[a].at[o], slot(a, c, 0, 0, 0), local.at[a]).start()
            else:
                landed(slot(a, c, t, 0, 0), take_a.at[t, a])
            for di, dy in steps:
                second(t, di, dy, a).start()
            third(t, 0, 0, a).start()
        if t > 0:
            relay(t - 1)
    relay(outer - 1)
    for a in range(count):
        pltpu.make_async_copy(ins[a].at[o], slot(a, c, 0, 0, 0), local.at[a]).wait()
        for d in range(1, outer):
            first(d, a).wait_send()
        for t in range(outer):
            for di, dy in [(0, 0)] + steps:
                landed(slot(a, 1 - c, t, di, dy), take_c.at[t, di, dy, a])
                third(t, di, dy, a).wait_send()
                if (di, dy) != (0, 0):
                    second(t, di, dy, a).wait_send()


def spread_rows(arrays, outer, inner, ys):
    count = len(arrays)
    outs = [
        jax.ShapeDtypeStruct((CORES, outer, inner, ys) + x.shape[1:], x.dtype) for x in arrays
    ]
    wide = DMA((outer, inner, ys, count))
    scratch = [DMA((count,)), DMA((outer, count)), DMA((outer, count)), wide, wide, wide, wide]
    return call(
        functools.partial(spread_kernel, outer, inner, ys, count), 3, outs, scratch, arrays
    )


def mate_kernel(pieces, source, target, send, take):
    place, tp = lax.axis_index("sp"), lax.axis_index("tp")
    y, c = tp // CORES, tp % CORES
    mate = (place, y * CORES + 1 - c)
    greet([mate])

    def copy(p):
        return remote(source.at[1 - c, p], target.at[p], send.at[p], take.at[p], mate)

    for p in range(pieces):
        copy(p).start()
    for p in range(pieces):
        copy(p).wait()


def plane_kernel(outer, inner, ys, source, target, send, take):
    place, tp = lax.axis_index("sp"), lax.axis_index("tp")
    o, i, y, c = place // inner, place % inner, tp // CORES, tp % CORES
    steps = [(di, dy) for di in range(inner) for dy in range(ys) if (di, dy) != (0, 0)]

    def beside(di, dy):
        return (o * inner + (i + di) % inner, (y + dy) % ys * CORES + c)

    greet([beside(di, dy) for di, dy in steps])

    def copy(n, k):
        di, dy = steps[n]
        return remote(
            source.at[k, (i + di) % inner, (y + dy) % ys],
            target.at[n, k],
            send.at[n, k],
            take.at[n, k],
            beside(di, dy),
        )

    for k in range(outer):
        for n in range(len(steps)):
            copy(n, k).start()
    for k in range(outer):
        for n in range(len(steps)):
            copy(n, k).wait()


def fast_body(
    residual,
    query_wide,
    key_wide,
    value_wide,
    query_narrow,
    key_narrow,
    value_narrow,
    gate_wide,
    gate_narrow,
    out_wide,
    out_narrow,
    norm_gain,
    routing,
    route_weight,
    gate_weight,
    up_weight,
    down_weight,
):
    inner = routing.shape[1]
    places = lax.axis_size("sp")
    outer = places // inner
    parts = lax.axis_size("tp")
    ys = parts // CORES
    core = lax.axis_index("tp") % CORES
    y = lax.axis_index("tp") // CORES
    i = lax.axis_index("sp") % inner
    own_rows, features = residual.shape

    gates = jnp.concatenate([gate_wide, gate_narrow], axis=1).T
    running = jnp.cumsum(jax.nn.log_sigmoid(gates), axis=1)
    heads = gates.shape[0]
    far = jnp.pad(running, ((0, -heads % 8), (0, 0)))
    keys_wide, values_wide, keys_narrow, values_narrow, far = gather_keys(
        [key_wide, value_wide, key_narrow, value_narrow, far], outer, inner
    )
    shard_rows, wide = query_wide.shape
    narrow = query_narrow.shape[1]
    att = pl.pallas_call(
        attend_kernel,
        out_shape=jax.ShapeDtypeStruct((shard_rows, wide + narrow), jnp.bfloat16),
        in_specs=[VMEM] * 8,
        out_specs=VMEM,
        scratch_shapes=[
            pltpu.VMEM((heads, shard_rows, 1), jnp.float32),
            pltpu.VMEM((heads, shard_rows, 1), jnp.float32),
            pltpu.VMEM((heads, shard_rows, wide), jnp.float32),
        ],
    )(
        query_wide,
        query_narrow,
        running.T,
        keys_wide,
        values_wide,
        keys_narrow,
        values_narrow,
        far,
    )
    att = swap(att.reshape(parts, own_rows, wide + narrow), "tp", parts, 1, 2)
    att_wide = jnp.transpose(att[:, :, :wide], (1, 0, 2)).reshape(own_rows, parts * wide)
    att_narrow = jnp.transpose(att[:, :, wide:], (1, 0, 2)).reshape(own_rows, parts * narrow)
    mixed = jnp.dot(att_wide, out_wide, preferred_element_type=jnp.float32)
    mixed = mixed + jnp.dot(att_narrow, out_narrow, preferred_element_type=jnp.float32)
    middle = (residual.astype(jnp.float32) + mixed).astype(jnp.bfloat16)
    middle_wide = middle.astype(jnp.float32)
    spread = jnp.mean(middle_wide * middle_wide, axis=1, keepdims=True)
    normed = (middle_wide * lax.rsqrt(spread + epsilon) * norm_gain).astype(jnp.bfloat16)

    capacity = own_rows * GROUPS // places
    group = routing[:, 0] // inner
    matches = (group[:, None] == jnp.arange(GROUPS, dtype=jnp.int32)[None, :]).astype(jnp.int32)
    ranking = jnp.sum((jnp.cumsum(matches, axis=0) - matches) * matches, axis=1)
    placing = group * capacity + ranking
    picker = placing[None, :] == jnp.arange(GROUPS * capacity, dtype=jnp.int32)[:, None]
    of_expert = jnp.sum(
        jnp.where(
            (routing % inner)[:, :, None] == jnp.arange(inner, dtype=jnp.int32)[None, None, :],
            route_weight[:, :, None],
            0.0,
        ),
        axis=1,
    )
    slot_weight = jnp.sum(jnp.where(picker[:, :, None], of_expert[None, :, :], 0.0), axis=1)
    slot_weight = jnp.pad(slot_weight, ((0, 0), (0, -inner % 128)))
    picker = picker.astype(jnp.bfloat16)
    outgoing = jnp.dot(picker, normed, preferred_element_type=jnp.float32).astype(jnp.bfloat16)
    pooled, pooled_weight = spread_rows(
        [
            outgoing.reshape(GROUPS, capacity, features),
            slot_weight.reshape(GROUPS, capacity, slot_weight.shape[1]),
        ],
        outer,
        inner,
        ys,
    )
    pooled = pooled.reshape(-1, features)
    pooled_weight = pooled_weight.reshape(pooled.shape[0], -1)
    scale = jnp.where(i == 0, pooled_weight[:, :1], 0.0)
    for other in range(1, inner):
        scale = jnp.where(i == other, pooled_weight[:, other : other + 1], scale)
    gate_value = jnp.dot(pooled, gate_weight[0], preferred_element_type=jnp.float32)
    up_value = jnp.dot(pooled, up_weight[0], preferred_element_type=jnp.float32)
    hidden = (jax.nn.silu(gate_value) * up_value).astype(jnp.bfloat16)
    answers = jnp.dot(hidden, down_weight[0], preferred_element_type=jnp.float32)
    answers = (answers * scale).astype(jnp.bfloat16)
    answers = answers.reshape(CORES, outer, inner, ys, capacity, features)
    half = jax.ShapeDtypeStruct(answers.shape[1:], jnp.bfloat16)
    arrived = call(
        functools.partial(mate_kernel, outer),
        4,
        [half],
        [DMA((outer,)), DMA((outer,))],
        [answers],
    )[0]
    own = lax.dynamic_index_in_dim(answers, core, 0, keepdims=False)
    chip = (own.astype(jnp.float32) + arrived.astype(jnp.float32)).astype(jnp.bfloat16)
    others = inner * ys - 1
    arrived = call(
        functools.partial(plane_kernel, outer, inner, ys),
        5,
        [jax.ShapeDtypeStruct((others, outer, capacity, features), jnp.bfloat16)],
        [DMA((others, outer)), DMA((others, outer))],
        [chip],
    )[0]
    own = lax.dynamic_slice(
        chip, (0, i, y, 0, 0), (outer, 1, 1, capacity, features)
    ).reshape(outer, capacity, features)
    plane = own.astype(jnp.float32) + jnp.sum(arrived.astype(jnp.float32), axis=0)
    returned = swap(plane.astype(jnp.bfloat16), "sp", outer, inner, 6)
    combined = jnp.dot(
        picker.T, returned.reshape(-1, features), preferred_element_type=jnp.float32
    )
    return (middle_wide + combined).astype(jnp.bfloat16)


def choose(*args):
    routing, gate_weight = args[12], args[14]
    experts = gate_weight.shape[0] * lax.axis_size("sp")
    paired = lax.axis_size("tp") % CORES == 0 and gate_weight.shape[0] == 1
    if paired and experts == GROUPS * routing.shape[1]:
        return fast_body(*args)
    return body(*args)


def solution(mesh):
    placed = (
        P(("sp", "tp"), None),
        P("sp", "tp"),
        P("sp", "tp"),
        P("sp", "tp"),
        P("sp", "tp"),
        P("sp", "tp"),
        P("sp", "tp"),
        P("sp", "tp"),
        P("sp", "tp"),
        P(),
        P(),
        P(),
        P(("sp", "tp"), None),
        P(("sp", "tp"), None),
        P("sp", None, "tp"),
        P("sp", None, "tp"),
        P("sp", "tp", None),
    )
    return jax.shard_map(
        choose, mesh=mesh, in_specs=placed, out_specs=P(("sp", "tp"), None), check_vma=False
    )
```

```python
import functools
import math

import jax
import jax.numpy as jnp
from jax import lax
from jax.experimental import pallas as pl
from jax.experimental.pallas import tpu as pltpu
from jax.sharding import PartitionSpec as P

HW = 128
HN = 64
GROUPS = 4


epsilon = 1e-06


def globalize(pieces, shard_rows):
    shards = pieces.shape[0] // shard_rows
    grid = pieces.reshape(shards, shard_rows, pieces.shape[1])
    endings = grid[:, -1, :]
    offsets = jnp.cumsum(endings, axis=0) - endings
    return (grid + offsets[:, None, :]).reshape(pieces.shape)


def head_block(
    state, queries, query_decay, keys, values, key_decay, first_key, first_query, head_width
):
    highest_old, weight_sum, weighted = state
    query_rows = queries.shape[0]
    head_count = query_decay.shape[1]
    key_rows = keys.shape[0]
    grid_query = queries.reshape(query_rows, head_count, head_width)
    grid_key = keys.reshape(key_rows, head_count, head_width)
    grid_value = values.reshape(key_rows, head_count, head_width)
    scores = jnp.einsum("thd,phd->htp", grid_query, grid_key, preferred_element_type=jnp.float32)
    scores = scores * head_width ** (-0.5) + query_decay.T[:, :, None] - key_decay.T[:, None, :]
    query_place = first_query + jnp.arange(query_rows, dtype=jnp.int32)
    key_place = first_key + jnp.arange(key_rows, dtype=jnp.int32)
    scores = jnp.where(key_place[None, None, :] <= query_place[None, :, None], scores, -jnp.inf)
    highest = jnp.maximum(highest_old, jnp.max(scores, axis=2))
    weights = jnp.exp(scores - highest[:, :, None])
    shrink = jnp.exp(highest_old - highest)
    weight_sum = weight_sum * shrink + jnp.sum(weights, axis=2)
    product = jnp.einsum(
        "htp,phd->htd", weights.astype(jnp.bfloat16), grid_value, preferred_element_type=jnp.float32
    )
    weighted = weighted * shrink[:, :, None] + product
    return (highest, weight_sum, weighted)


def fresh_state(head_count, shard_rows, head_width):
    return (
        jnp.full((head_count, shard_rows), -1e30, jnp.float32),
        jnp.zeros((head_count, shard_rows), jnp.float32),
        jnp.zeros((head_count, shard_rows, head_width), jnp.float32),
    )


def finish(state, shard_rows):
    highest, weight_sum, weighted = state
    mixed_heads = weighted / weight_sum[:, :, None]
    joined = jnp.transpose(mixed_heads, (1, 0, 2))
    return joined.reshape(shard_rows, weighted.shape[0] * weighted.shape[2]).astype(jnp.bfloat16)


def body(
    residual,
    query_wide,
    key_wide,
    value_wide,
    query_narrow,
    key_narrow,
    value_narrow,
    gate_wide,
    gate_narrow,
    out_wide,
    out_narrow,
    norm_gain,
    routing,
    route_weight,
    gate_weight,
    up_weight,
    down_weight,
):
    shard_rows = query_wide.shape[0]
    half_rows = shard_rows // 2
    sp_place = lax.axis_index("sp")
    first_query = sp_place * shard_rows
    running_wide = jnp.cumsum(jax.nn.log_sigmoid(gate_wide), axis=0)
    running_narrow = jnp.cumsum(jax.nn.log_sigmoid(gate_narrow), axis=0)
    pieces_wide, pieces_narrow = (
        lax.all_gather(running_wide, "sp", axis=0, tiled=True),
        lax.all_gather(running_narrow, "sp", axis=0, tiled=True),
    )
    every_wide = globalize(pieces_wide, shard_rows)
    every_narrow = globalize(pieces_narrow, shard_rows)
    late_first = first_query + half_rows
    halves = []
    for place, part_wide, part_narrow in (
        (first_query, query_wide[:half_rows], query_narrow[:half_rows]),
        (late_first, query_wide[half_rows:], query_narrow[half_rows:]),
    ):
        halves.append(
            (
                place,
                part_wide,
                part_narrow,
                lax.dynamic_slice_in_dim(every_wide, place, half_rows, 0),
                lax.dynamic_slice_in_dim(every_narrow, place, half_rows, 0),
            )
        )

    def half_state():
        return (
            fresh_state(gate_wide.shape[1], half_rows, HW),
            fresh_state(gate_narrow.shape[1], half_rows, HN),
        )

    state = (half_state(), half_state())
    keys_wide = lax.all_gather(key_wide, "sp", axis=0, tiled=True)
    values_wide = lax.all_gather(value_wide, "sp", axis=0, tiled=True)
    keys_narrow = lax.all_gather(key_narrow, "sp", axis=0, tiled=True)
    values_narrow = lax.all_gather(value_narrow, "sp", axis=0, tiled=True)
    span_rows = keys_wide.shape[0]
    block_size = math.gcd(span_rows, 2048)

    def visit(carried, position):
        inside = position * block_size

        def take_block(source):
            return lax.dynamic_slice_in_dim(source, inside, block_size, 0)

        def take_decay(source):
            return lax.dynamic_slice_in_dim(source, inside, block_size, 0)

        block_kw = take_block(keys_wide)
        block_vw = take_block(values_wide)
        block_kn = take_block(keys_narrow)
        block_vn = take_block(values_narrow)
        block_dw = take_decay(every_wide)
        block_dn = take_decay(every_narrow)

        def one_half(current, half):
            place, part_wide, part_narrow, query_decay_wide, query_decay_narrow = half

            def work(inner):
                first = head_block(
                    inner[0],
                    part_wide,
                    query_decay_wide,
                    block_kw,
                    block_vw,
                    block_dw,
                    inside,
                    place,
                    HW,
                )
                second = head_block(
                    inner[1],
                    part_narrow,
                    query_decay_narrow,
                    block_kn,
                    block_vn,
                    block_dn,
                    inside,
                    place,
                    HN,
                )
                return (first, second)

            def skip(inner):
                return inner

            return lax.cond(inside <= place + half_rows - 1, work, skip, current)

        updated = (one_half(carried[0], halves[0]), one_half(carried[1], halves[1]))
        return (updated, None)

    state, _ = lax.scan(visit, state, jnp.arange(span_rows // block_size, dtype=jnp.int32))
    att_wide = jnp.concatenate(
        [finish(state[0][0], half_rows), finish(state[1][0], half_rows)], axis=0
    )
    att_narrow = jnp.concatenate(
        [finish(state[0][1], half_rows), finish(state[1][1], half_rows)], axis=0
    )
    own_rows = residual.shape[0]
    tp_place = lax.axis_index("tp")
    rows_wide = lax.dynamic_slice_in_dim(
        out_wide, tp_place * att_wide.shape[1], att_wide.shape[1], 0
    )
    rows_narrow = lax.dynamic_slice_in_dim(
        out_narrow, tp_place * att_narrow.shape[1], att_narrow.shape[1], 0
    )
    first = jnp.dot(att_wide, rows_wide, preferred_element_type=jnp.float32)
    second = jnp.dot(att_narrow, rows_narrow, preferred_element_type=jnp.float32)
    mixed = lax.psum_scatter(
        (first + second).astype(jnp.bfloat16), "tp", scatter_dimension=0, tiled=True
    ).astype(jnp.float32)
    middle = (residual.astype(jnp.float32) + mixed).astype(jnp.bfloat16)
    middle_wide = middle.astype(jnp.float32)
    spread = jnp.mean(middle_wide * middle_wide, axis=1, keepdims=True)
    normed = (middle_wide * lax.rsqrt(spread + epsilon) * norm_gain).astype(jnp.bfloat16)
    features = normed.shape[1]
    chosen_count = routing.shape[1]
    expert_count = gate_weight.shape[0] * lax.axis_size("sp")
    capacity = own_rows * GROUPS // expert_count
    flat_routes = routing.reshape(-1)
    matches = (flat_routes[:, None] == jnp.arange(expert_count, dtype=jnp.int32)[None, :]).astype(
        jnp.int32
    )
    ranking = jnp.sum((jnp.cumsum(matches, axis=0) - matches) * matches, axis=1)
    placing = flat_routes * capacity + ranking
    picker = (
        placing[None, :] == jnp.arange(expert_count * capacity, dtype=jnp.int32)[:, None]
    ).astype(jnp.bfloat16)
    picker = jnp.sum(picker.reshape(expert_count * capacity, own_rows, chosen_count), axis=2)
    outgoing = jnp.dot(picker, normed, preferred_element_type=jnp.float32).astype(jnp.bfloat16)
    outgoing = outgoing.reshape(expert_count, capacity, features)
    arrived = lax.all_to_all(outgoing, "sp", split_axis=0, concat_axis=0, tiled=True)
    pooled = lax.all_gather(arrived.reshape(-1, features), "tp", axis=0, tiled=True)
    gate_value = jnp.dot(pooled, gate_weight[0], preferred_element_type=jnp.float32)
    up_value = jnp.dot(pooled, up_weight[0], preferred_element_type=jnp.float32)
    hidden = (jax.nn.silu(gate_value) * up_value).astype(jnp.bfloat16)
    answers = lax.psum_scatter(
        jnp.dot(hidden, down_weight[0], preferred_element_type=jnp.float32).astype(jnp.bfloat16),
        "tp",
        scatter_dimension=0,
        tiled=True,
    )
    returned = lax.all_to_all(
        answers.reshape(expert_count, capacity, features),
        "sp",
        split_axis=0,
        concat_axis=0,
        tiled=True,
    )
    picked = jnp.take(returned.reshape(expert_count * capacity, features), placing, axis=0)
    picked = picked.reshape(own_rows, chosen_count, features).astype(jnp.float32)
    combined = jnp.sum(route_weight[:, :, None] * picked, axis=1)
    return (middle_wide + combined).astype(jnp.bfloat16)


CORES = 2
MESH = pl.DeviceIdType.MESH
VMEM = pl.BlockSpec(memory_space=pltpu.VMEM)


def greet(peers):
    barrier = pltpu.get_barrier_semaphore()
    for peer in peers:
        pl.semaphore_signal(barrier, inc=1, device_id=peer, device_id_type=MESH)
    pl.semaphore_wait(barrier, len(peers))


def remote(source, target, send, receive, peer):
    return pltpu.make_async_remote_copy(
        src_ref=source,
        dst_ref=target,
        send_sem=send,
        recv_sem=receive,
        device_id=peer,
        device_id_type=MESH,
    )


def call(kernel, number, outs, scratch, args):
    return pl.pallas_call(
        kernel,
        out_shape=outs,
        in_specs=[VMEM] * len(args),
        out_specs=[VMEM] * len(outs),
        scratch_shapes=scratch,
        compiler_params=pltpu.CompilerParams(collective_id=number, has_side_effects=True),
    )(*args)


DMA = pltpu.SemaphoreType.DMA


def keys_kernel(outer, inner, count, *refs):
    ins, outs = refs[:count], refs[count : 2 * count]
    local, send_up, take_up, send_in, take_in = refs[2 * count :]
    place = lax.axis_index("sp")
    o, i = place // inner, place % inner
    tp = lax.axis_index("tp")

    def at(o_, i_):
        return (o_ * inner + i_, tp)

    greet(
        [at((o + d) % outer, i) for d in range(1, outer)]
        + [at(o, (i + d) % inner) for d in range(1, inner)]
    )
    other = at((o + 1) % outer, i)

    def up(t, a):
        slot = (o - t) * inner + i
        source = ins[a] if t == 0 else outs[a].at[slot]
        return remote(source, outs[a].at[slot], send_up.at[t, a], take_up.at[t, a], at(o + 1, i))

    def across(t, d, a):
        slot = (o - t) * inner + i
        source = ins[a] if t == 0 else outs[a].at[slot]
        return remote(
            source,
            outs[a].at[slot],
            send_in.at[t, d - 1, a],
            take_in.at[t, d - 1, a],
            at(o, (i + d) % inner),
        )

    def landed(slot, a, semaphore):
        remote(outs[a].at[slot], outs[a].at[slot], semaphore, semaphore, other).wait_recv()

    for a in range(count):
        pltpu.make_async_copy(ins[a], outs[a].at[place], local.at[a]).start()
    for t in range(outer):

        @pl.when(o >= t)
        def _(t=t):
            for a in range(count):
                if t > 0:
                    landed((o - t) * inner + i, a, take_up.at[t - 1, a])
                if t < outer - 1:

                    @pl.when(o + 1 < outer)
                    def _(a=a):
                        up(t, a).start()

                for d in range(1, inner):
                    if t > 0:
                        across(t, d, a).start()
                    else:

                        @pl.when((i + d) % inner > i)
                        def _(a=a, d=d):
                            across(t, d, a).start()

    for t in range(outer):

        @pl.when(o >= t)
        def _(t=t):
            for a in range(count):
                for d in range(1, inner):
                    giver = (i - d + inner) % inner
                    slot = (o - t) * inner + giver
                    if t > 0:
                        landed(slot, a, take_in.at[t, d - 1, a])
                        across(t, d, a).wait_send()
                    else:

                        @pl.when(giver < i)
                        def _(a=a, d=d, slot=slot):
                            landed(slot, a, take_in.at[0, d - 1, a])

                        @pl.when((i + d) % inner > i)
                        def _(a=a, d=d):
                            across(0, d, a).wait_send()

                if t < outer - 1:

                    @pl.when(o + 1 < outer)
                    def _(a=a):
                        up(t, a).wait_send()

    for a in range(count):
        pltpu.make_async_copy(ins[a], outs[a].at[place], local.at[a]).wait()


def gather_keys(arrays, outer, inner):
    count = len(arrays)
    outs = [jax.ShapeDtypeStruct((outer * inner,) + x.shape, x.dtype) for x in arrays]
    scratch = [
        DMA((count,)),
        DMA((outer, count)),
        DMA((outer, count)),
        DMA((outer, inner, count)),
        DMA((outer, inner, count)),
    ]
    return call(functools.partial(keys_kernel, outer, inner, count), 1, outs, scratch, arrays)


def attend_kernel(qw, qn, near, kw, vw, kn, vn, far, out, top, total, mixed):
    place = lax.axis_index("sp")
    rows = qw.shape[0]
    width = qn.shape[1]
    heads = 1 + width // HN
    lanes = lax.broadcasted_iota(jnp.int32, (rows, width), 1) // HN

    def query(h):
        if h == 0:
            return qw[...]
        return jnp.where(lanes == h - 1, qn[...], jnp.zeros_like(qn[...]))

    def block(j, shift, diagonal):
        for h in range(heads):
            keys, values = (kw, vw) if h == 0 else (kn, vn)
            size = HW if h == 0 else HN
            scores = lax.dot_general(
                query(h), keys[j], (((1,), (1,)), ((), ())), preferred_element_type=jnp.float32
            )
            drop = (near[:, h : h + 1] + shift[h]) - far[j, h : h + 1, :]
            scores = scores * size ** (-0.5) + drop
            if diagonal:
                t = lax.broadcasted_iota(jnp.int32, scores.shape, 0)
                s = lax.broadcasted_iota(jnp.int32, scores.shape, 1)
                scores = jnp.where(s <= t, scores, -jnp.inf)
            peak = jnp.max(scores, axis=1, keepdims=True)
            if diagonal:
                weights = jnp.exp(scores - peak)
                total[h] = jnp.sum(weights, axis=1, keepdims=True)
                mixed[h] = jnp.dot(
                    weights.astype(jnp.bfloat16), values[j], preferred_element_type=jnp.float32
                )
                top[h] = peak
            else:
                before = top[h]
                peak = jnp.maximum(before, peak)
                weights = jnp.exp(scores - peak)
                shrink = jnp.exp(before - peak)
                total[h] = total[h] * shrink + jnp.sum(weights, axis=1, keepdims=True)
                mixed[h] = mixed[h] * shrink + jnp.dot(
                    weights.astype(jnp.bfloat16), values[j], preferred_element_type=jnp.float32
                )
                top[h] = peak

    block(place, [jnp.zeros((1, 1), jnp.float32)] * heads, True)

    def step(t, shift):
        j = place - 1 - t
        shift = tuple(shift[h] + far[j, h : h + 1, rows - 1 : rows] for h in range(heads))
        block(j, shift, False)
        return shift

    lax.fori_loop(0, place, step, tuple(jnp.zeros((1, 1), jnp.float32) for _ in range(heads)))
    out[:, : qw.shape[1]] = (mixed[0] / total[0]).astype(jnp.bfloat16)
    narrow = mixed[1] / total[1]
    for h in range(2, heads):
        narrow = jnp.where(lanes == h - 1, mixed[h] / total[h], narrow)
    out[:, qw.shape[1] :] = narrow.astype(jnp.bfloat16)


def swap_kernel(axis, n, stride, source, target, local, send, take):
    sp, tp = lax.axis_index("sp"), lax.axis_index("tp")
    me = (sp if axis == "sp" else tp) // stride
    rest = (sp if axis == "sp" else tp) % stride

    def at(k):
        return (k * stride + rest, tp) if axis == "sp" else (sp, k * stride + rest)

    greet([at((me + d) % n) for d in range(1, n)])

    def copy(d):
        k = (me + d) % n
        return remote(source.at[k], target.at[me], send.at[d], take.at[d], at(k))

    for d in range(1, n):
        copy(d).start()
    own = pltpu.make_async_copy(source.at[me], target.at[me], local.at[0])
    own.start()
    own.wait()
    for d in range(1, n):
        slot = target.at[(me - d + n) % n]
        remote(slot, slot, send.at[d], take.at[d], at((me + d) % n)).wait_recv()
        copy(d).wait_send()


def swap(array, axis, n, stride, number):
    return call(
        functools.partial(swap_kernel, axis, n, stride),
        number,
        [jax.ShapeDtypeStruct(array.shape, array.dtype)],
        [DMA((1,)), DMA((n,)), DMA((n,))],
        [array],
    )[0]


def spread_kernel(outer, inner, ys, count, *refs):
    ins, outs = refs[:count], refs[count : 2 * count]
    local, send_a, take_a, send_b, take_b, send_c, take_c = refs[2 * count :]
    place, tp = lax.axis_index("sp"), lax.axis_index("tp")
    o, i, y, c = place // inner, place % inner, tp // CORES, tp % CORES
    steps = [(di, dy) for di in range(inner) for dy in range(ys) if (di, dy) != (0, 0)]
    mate = (place, y * CORES + 1 - c)

    def beside(di, dy):
        return (o * inner + (i + di) % inner, (y + dy) % ys * CORES + c)

    def above(d):
        return ((o + d) % outer * inner + i, tp)

    greet(
        [above(d) for d in range(1, outer)] + [beside(di, dy) for di, dy in steps] + [mate]
    )

    def slot(a, core, t, di, dy):
        return outs[a].at[
            core, (o - t + outer) % outer, (i - di + inner) % inner, (y - dy + ys) % ys
        ]

    def first(d, a):
        return remote(
            ins[a].at[(o + d) % outer],
            outs[a].at[c, o, i, y],
            send_a.at[d, a],
            take_a.at[d, a],
            above(d),
        )

    def second(t, di, dy, a):
        source = ins[a].at[o] if t == 0 else slot(a, c, t, 0, 0)
        return remote(
            source,
            slot(a, c, t, 0, 0),
            send_b.at[t, di, dy, a],
            take_b.at[t, di, dy, a],
            beside(di, dy),
        )

    def third(t, di, dy, a):
        source = ins[a].at[o] if (t, di, dy) == (0, 0, 0) else slot(a, c, t, di, dy)
        return remote(
            source, slot(a, c, t, di, dy), send_c.at[t, di, dy, a], take_c.at[t, di, dy, a], mate
        )

    def landed(where, semaphore):
        remote(where, where, semaphore, semaphore, mate).wait_recv()

    def relay(t):
        for di, dy in steps:
            for a in range(count):
                landed(slot(a, c, t, di, dy), take_b.at[t, di, dy, a])
                third(t, di, dy, a).start()

    for d in range(1, outer):
        for a in range(count):
            first(d, a).start()
    for t in range(outer):
        for a in range(count):
            if t == 0:
                pltpu.make_async_copy(ins[a].at[o], slot(a, c, 0, 0, 0), local.at[a]).start()
            else:
                landed(slot(a, c, t, 0, 0), take_a.at[t, a])
            for di, dy in reversed(steps):
                second(t, di, dy, a).start()
            third(t, 0, 0, a).start()
        if t > 0:
            relay(t - 1)
    relay(outer - 1)
    for a in range(count):
        pltpu.make_async_copy(ins[a].at[o], slot(a, c, 0, 0, 0), local.at[a]).wait()
        for d in range(1, outer):
            first(d, a).wait_send()
        for t in range(outer):
            for di, dy in [(0, 0)] + steps:
                landed(slot(a, 1 - c, t, di, dy), take_c.at[t, di, dy, a])
                third(t, di, dy, a).wait_send()
                if (di, dy) != (0, 0):
                    second(t, di, dy, a).wait_send()


def spread_rows(arrays, outer, inner, ys):
    count = len(arrays)
    outs = [
        jax.ShapeDtypeStruct((CORES, outer, inner, ys) + x.shape[1:], x.dtype) for x in arrays
    ]
    wide = DMA((outer, inner, ys, count))
    scratch = [DMA((count,)), DMA((outer, count)), DMA((outer, count)), wide, wide, wide, wide]
    return call(
        functools.partial(spread_kernel, outer, inner, ys, count), 3, outs, scratch, arrays
    )


def mate_kernel(pieces, source, target, send, take):
    place, tp = lax.axis_index("sp"), lax.axis_index("tp")
    y, c = tp // CORES, tp % CORES
    mate = (place, y * CORES + 1 - c)
    greet([mate])

    def copy(p):
        return remote(source.at[1 - c, p], target.at[p], send.at[p], take.at[p], mate)

    for p in range(pieces):
        copy(p).start()
    for p in range(pieces):
        copy(p).wait()


def plane_kernel(outer, inner, ys, source, target, send, take):
    place, tp = lax.axis_index("sp"), lax.axis_index("tp")
    o, i, y, c = place // inner, place % inner, tp // CORES, tp % CORES
    steps = [(di, dy) for di in range(inner) for dy in range(ys) if (di, dy) != (0, 0)]

    def beside(di, dy):
        return (o * inner + (i + di) % inner, (y + dy) % ys * CORES + c)

    greet([beside(di, dy) for di, dy in steps])

    def copy(n, k):
        di, dy = steps[n]
        return remote(
            source.at[k, (i + di) % inner, (y + dy) % ys],
            target.at[n, k],
            send.at[n, k],
            take.at[n, k],
            beside(di, dy),
        )

    for k in range(outer):
        for n in reversed(range(len(steps))):
            copy(n, k).start()
    for k in range(outer):
        for n in range(len(steps)):
            copy(n, k).wait()


def fast_body(
    residual,
    query_wide,
    key_wide,
    value_wide,
    query_narrow,
    key_narrow,
    value_narrow,
    gate_wide,
    gate_narrow,
    out_wide,
    out_narrow,
    norm_gain,
    routing,
    route_weight,
    gate_weight,
    up_weight,
    down_weight,
):
    inner = routing.shape[1]
    places = lax.axis_size("sp")
    outer = places // inner
    parts = lax.axis_size("tp")
    ys = parts // CORES
    core = lax.axis_index("tp") % CORES
    y = lax.axis_index("tp") // CORES
    i = lax.axis_index("sp") % inner
    own_rows, features = residual.shape

    gates = jnp.concatenate([gate_wide, gate_narrow], axis=1).T
    running = jnp.cumsum(jax.nn.log_sigmoid(gates), axis=1)
    heads = gates.shape[0]
    far = jnp.pad(running, ((0, -heads % 8), (0, 0)))
    keys_wide, values_wide, keys_narrow, values_narrow, far = gather_keys(
        [key_wide, value_wide, key_narrow, value_narrow, far], outer, inner
    )
    shard_rows, wide = query_wide.shape
    narrow = query_narrow.shape[1]
    att = pl.pallas_call(
        attend_kernel,
        out_shape=jax.ShapeDtypeStruct((shard_rows, wide + narrow), jnp.bfloat16),
        in_specs=[VMEM] * 8,
        out_specs=VMEM,
        scratch_shapes=[
            pltpu.VMEM((heads, shard_rows, 1), jnp.float32),
            pltpu.VMEM((heads, shard_rows, 1), jnp.float32),
            pltpu.VMEM((heads, shard_rows, wide), jnp.float32),
        ],
    )(
        query_wide,
        query_narrow,
        running.T,
        keys_wide,
        values_wide,
        keys_narrow,
        values_narrow,
        far,
    )
    att = swap(att.reshape(parts, own_rows, wide + narrow), "tp", parts, 1, 2)
    att_wide = jnp.transpose(att[:, :, :wide], (1, 0, 2)).reshape(own_rows, parts * wide)
    att_narrow = jnp.transpose(att[:, :, wide:], (1, 0, 2)).reshape(own_rows, parts * narrow)
    mixed = jnp.dot(att_wide, out_wide, preferred_element_type=jnp.float32)
    mixed = mixed + jnp.dot(att_narrow, out_narrow, preferred_element_type=jnp.float32)
    middle = (residual.astype(jnp.float32) + mixed).astype(jnp.bfloat16)
    middle_wide = middle.astype(jnp.float32)
    spread = jnp.mean(middle_wide * middle_wide, axis=1, keepdims=True)
    normed = (middle_wide * lax.rsqrt(spread + epsilon) * norm_gain).astype(jnp.bfloat16)

    capacity = own_rows * GROUPS // places
    group = routing[:, 0] // inner
    matches = (group[:, None] == jnp.arange(GROUPS, dtype=jnp.int32)[None, :]).astype(jnp.int32)
    ranking = jnp.sum((jnp.cumsum(matches, axis=0) - matches) * matches, axis=1)
    placing = group * capacity + ranking
    picker = placing[None, :] == jnp.arange(GROUPS * capacity, dtype=jnp.int32)[:, None]
    of_expert = jnp.sum(
        jnp.where(
            (routing % inner)[:, :, None] == jnp.arange(inner, dtype=jnp.int32)[None, None, :],
            route_weight[:, :, None],
            0.0,
        ),
        axis=1,
    )
    slot_weight = jnp.sum(jnp.where(picker[:, :, None], of_expert[None, :, :], 0.0), axis=1)
    slot_weight = jnp.pad(slot_weight, ((0, 0), (0, -inner % 128)))
    picker = picker.astype(jnp.bfloat16)
    outgoing = jnp.dot(picker, normed, preferred_element_type=jnp.float32).astype(jnp.bfloat16)
    pooled, pooled_weight = spread_rows(
        [
            outgoing.reshape(GROUPS, capacity, features),
            slot_weight.reshape(GROUPS, capacity, slot_weight.shape[1]),
        ],
        outer,
        inner,
        ys,
    )
    pooled = pooled.reshape(-1, features)
    pooled_weight = pooled_weight.reshape(pooled.shape[0], -1)
    scale = jnp.where(i == 0, pooled_weight[:, :1], 0.0)
    for other in range(1, inner):
        scale = jnp.where(i == other, pooled_weight[:, other : other + 1], scale)
    gate_value = jnp.dot(pooled, gate_weight[0], preferred_element_type=jnp.float32)
    up_value = jnp.dot(pooled, up_weight[0], preferred_element_type=jnp.float32)
    hidden = (jax.nn.silu(gate_value) * up_value).astype(jnp.bfloat16)
    answers = jnp.dot(hidden, down_weight[0], preferred_element_type=jnp.float32)
    answers = (answers * scale).astype(jnp.bfloat16)
    answers = answers.reshape(CORES, outer, inner, ys, capacity, features)
    half = jax.ShapeDtypeStruct(answers.shape[1:], jnp.bfloat16)
    arrived = call(
        functools.partial(mate_kernel, outer),
        4,
        [half],
        [DMA((outer,)), DMA((outer,))],
        [answers],
    )[0]
    own = lax.dynamic_index_in_dim(answers, core, 0, keepdims=False)
    chip = (own.astype(jnp.float32) + arrived.astype(jnp.float32)).astype(jnp.bfloat16)
    others = inner * ys - 1
    arrived = call(
        functools.partial(plane_kernel, outer, inner, ys),
        5,
        [jax.ShapeDtypeStruct((others, outer, capacity, features), jnp.bfloat16)],
        [DMA((others, outer)), DMA((others, outer))],
        [chip],
    )[0]
    own = lax.dynamic_slice(
        chip, (0, i, y, 0, 0), (outer, 1, 1, capacity, features)
    ).reshape(outer, capacity, features)
    plane = own.astype(jnp.float32) + jnp.sum(arrived.astype(jnp.float32), axis=0)
    returned = swap(plane.astype(jnp.bfloat16), "sp", outer, inner, 6)
    combined = jnp.dot(
        picker.T, returned.reshape(-1, features), preferred_element_type=jnp.float32
    )
    return (middle_wide + combined).astype(jnp.bfloat16)


def choose(*args):
    routing, gate_weight = args[12], args[14]
    experts = gate_weight.shape[0] * lax.axis_size("sp")
    paired = lax.axis_size("tp") % CORES == 0 and gate_weight.shape[0] == 1
    if paired and experts == GROUPS * routing.shape[1]:
        return fast_body(*args)
    return body(*args)


def solution(mesh):
    placed = (
        P(("sp", "tp"), None),
        P("sp", "tp"),
        P("sp", "tp"),
        P("sp", "tp"),
        P("sp", "tp"),
        P("sp", "tp"),
        P("sp", "tp"),
        P("sp", "tp"),
        P("sp", "tp"),
        P(),
        P(),
        P(),
        P(("sp", "tp"), None),
        P(("sp", "tp"), None),
        P("sp", None, "tp"),
        P("sp", None, "tp"),
        P("sp", "tp", None),
    )
    return jax.shard_map(
        choose, mesh=mesh, in_specs=placed, out_specs=P(("sp", "tp"), None), check_vma=False
    )
```
